32 devices in a mesh: sp: 16 (over z, y, x), tp: 2 (over core).
Axes of the slice: x: 2, y: 2, z: 4, core: 2. Of those that a mesh axis runs over, the one named last changes fastest.
Arguments:
- tokens: bfloat16 [2048, 2048], P('sp', 'tp'), may hold values from -6 to 6
- norm_gain: float32 [2048], replicated, may hold values from 0.1 to 1.9
- w_value: bfloat16 [2048, 2048], P('sp', 'tp'), may hold values from -0.125 to 0.125
- w_gate: bfloat16 [2048, 2048], P('sp', 'tp'), may hold values from -0.125 to 0.125
- conv_taps: bfloat16 [31, 2048], P(None, 'tp'), may hold values from -1 to 1
- conv_gain: float32 [2048], P('tp'), may hold values from 0.1 to 1.9
- w_query: bfloat16 [2048, 3072], P(None, 'tp'), may hold values from -5.303301 to 5.303301
- latent_down_weight: bfloat16 [2048, 512], P('sp'), may hold values from -0.125 to 0.125
- latent_norm_gain: float32 [512], replicated, may hold values from 0.1 to 1.9
- w_rope_key: bfloat16 [2048, 64], P('sp'), may hold values from -0.125 to 0.125
- key_up_weight: bfloat16 [512, 2048], P(None, 'tp'), may hold values from -0.5 to 0.5
- value_up_weight: bfloat16 [512, 2048], P(None, 'tp'), may hold values from -0.25 to 0.25
- w_merge_conv: bfloat16 [2048, 2048], P('tp'), may hold values from -0.09375 to 0.09375
- w_merge_attn: bfloat16 [2048, 2048], P('tp'), may hold values from -0.28125 to 0.28125
Outputs:
- merged: bfloat16 [2048, 2048], P(('sp', 'tp'))
- log_sums: float32 [2048, 16], P('sp', 'tp')
The draws below stay inside these ranges and needn't reach their ends.
All inputs are finite; a program needn't handle non-finite values.
Results may differ from the reference program's by a relative error of at most 0.025.
The reference program's roundings to bfloat16 on the way count: a program that leaves them out, or rounds other values in their place, can miss the bound.
Values may be sent and summed in bfloat16 or wider, within the bound.
A program may use at most 64 MiB of HBM per device.

```python
import jax
import jax.numpy as jnp
from jax import lax

MODEL_WIDTH = 2048
CC = 2048
HEAD_TOTAL = 16
KEY_VALUE_RANK = 512
PLAIN_QK_WIDTH = 128
QK_ROPE = 64
VALUE_HEAD_WIDTH = 128
CONV_WIDTH = 31
TOKEN_TOTAL = 2048
N_TP = 2


def draw_w_query(key, part):
    values = jnp.clip(jax.random.normal(key, (MODEL_WIDTH, HEAD_TOTAL * (PLAIN_QK_WIDTH + QK_ROPE)), jnp.float32), -6.0, 6.0) * MODEL_WIDTH ** (-0.5)
    return values.astype(jnp.bfloat16)


def block_scale(rng, shape, split, smallest, largest):
    level, own = 1.0, jax.random.fold_in(rng, 6)
    for axis_at, blocks in split:
        heights = jnp.exp(jax.random.uniform(jax.random.fold_in(own, axis_at), (blocks,), jnp.float32, smallest / len(split), largest / len(split)))
        level = level * jnp.repeat(heights, shape[axis_at] // blocks).reshape([-1 if axis == axis_at else 1 for axis in range(len(shape))])
    return level


def normal_values(own_key, extent, scale, limit, pieces=(), held_as=jnp.bfloat16):
    array = scale * jax.random.normal(own_key, extent, jnp.float32)
    if pieces:
        array = array * block_scale(own_key, extent, pieces, -0.22, 0.18)
    return jnp.clip(array, -limit, limit).astype(held_as)


def setup_inputs(seed: int = 0) -> dict:
    seeds = jax.random.split(jax.random.key(seed), 15)
    return {
        "tokens": normal_values(seeds[0], (TOKEN_TOTAL, MODEL_WIDTH), 1.0, 6.0, ((0, 16), (1, 2))),
        "norm_gain": jnp.clip(1.0 + 0.18 * jax.random.normal(seeds[1], (MODEL_WIDTH,), jnp.float32), 0.1, 1.9),
        "w_value": normal_values(seeds[2], (MODEL_WIDTH, CC), MODEL_WIDTH ** -0.5, 0.125, ((0, 16), (1, 2))),
        "w_gate": normal_values(seeds[3], (MODEL_WIDTH, CC), MODEL_WIDTH ** -0.5, 0.125, ((0, 16), (1, 2))),
        "conv_taps": normal_values(seeds[4], (CONV_WIDTH, CC), CONV_WIDTH ** -0.5, 1.0, ((1, 2),)),
        "conv_gain": jnp.clip(1.0 + 0.18 * jax.random.normal(seeds[5], (CC,), jnp.float32), 0.1, 1.9),
        "w_query": draw_w_query(jax.random.fold_in(seeds[14], 71), 0),
        "latent_down_weight": normal_values(seeds[7], (MODEL_WIDTH, KEY_VALUE_RANK), MODEL_WIDTH ** -0.5, 0.125, ((0, 16),)),
        "latent_norm_gain": jnp.clip(1.0 + 0.18 * jax.random.normal(seeds[8], (KEY_VALUE_RANK,), jnp.float32), 0.1, 1.9),
        "w_rope_key": normal_values(seeds[9], (MODEL_WIDTH, QK_ROPE), MODEL_WIDTH ** -0.5, 0.125, ((0, 16),)),
        "key_up_weight": normal_values(seeds[10], (KEY_VALUE_RANK, HEAD_TOTAL * PLAIN_QK_WIDTH), PLAIN_QK_WIDTH ** -0.5, 0.5, ((1, 2),)),
        "value_up_weight": normal_values(seeds[11], (KEY_VALUE_RANK, HEAD_TOTAL * VALUE_HEAD_WIDTH), KEY_VALUE_RANK ** -0.5, 0.25, ((1, 2),)),
        "w_merge_conv": normal_values(seeds[12], (CC, MODEL_WIDTH), (CC + HEAD_TOTAL * VALUE_HEAD_WIDTH) ** -0.5, 0.09375, ((0, 2),)),
        "w_merge_attn": normal_values(seeds[13], (HEAD_TOTAL * VALUE_HEAD_WIDTH, MODEL_WIDTH), (3.0 / (CC + HEAD_TOTAL * VALUE_HEAD_WIDTH) ** 0.5), 0.28125, ((0, 2),)),
    }


epsilon = 1e-06
rope_base = 10000.0
masked_score = -1e+30

def angles_at(positions, width):
    inverse = rope_base ** (-2.0 * jnp.arange(width // 2, dtype=jnp.float32) / width)
    return positions[:, None] * inverse[None, :]

def rotate(halves, angle):
    middle = halves.shape[-1] // 2
    first, second = (halves[..., :middle], halves[..., middle:])
    cosine, sine = (jnp.cos(angle), jnp.sin(angle))
    return jnp.concatenate([first * cosine - second * sine, first * sine + second * cosine], axis=-1)

def reference(tokens, norm_gain, w_value, w_gate, conv_taps, conv_gain, w_query, latent_down_weight, latent_norm_gain, w_rope_key, key_up_weight, value_up_weight, w_merge_conv, w_merge_attn):
    features = tokens.astype(jnp.float32)
    normed = (features * lax.rsqrt(lax.optimization_barrier(jnp.mean(features * features, axis=-1, keepdims=True)) + epsilon) * norm_gain).astype(jnp.bfloat16)
    value_pre = jnp.dot(normed, w_value, preferred_element_type=jnp.float32)
    gate_pre = jnp.dot(normed, w_gate, preferred_element_type=jnp.float32)
    gated_rows = (value_pre * jax.nn.sigmoid(gate_pre)).astype(jnp.bfloat16)
    conv_reach = CONV_WIDTH - 1
    padded = jnp.concatenate([jnp.zeros((conv_reach, CC), jnp.bfloat16), gated_rows], axis=0).astype(jnp.float32)
    mixed = jnp.zeros((TOKEN_TOTAL, CC), jnp.float32)
    for tap_index in range(CONV_WIDTH):
        mixed = mixed + conv_taps[tap_index].astype(jnp.float32) * padded[tap_index:tap_index + TOKEN_TOTAL]
    channel_mean = lax.optimization_barrier(jnp.mean(mixed, axis=-1, keepdims=True))
    channel_var = lax.optimization_barrier(jnp.mean(jnp.square(mixed - channel_mean), axis=-1, keepdims=True))
    conv_out = jax.nn.silu((mixed - channel_mean) * lax.rsqrt(channel_var + epsilon) * conv_gain).astype(jnp.bfloat16)
    positions = jnp.arange(TOKEN_TOTAL, dtype=jnp.float32)
    rope_angles = angles_at(positions, QK_ROPE)
    query = jnp.dot(normed, w_query, preferred_element_type=jnp.float32).astype(jnp.bfloat16).reshape(TOKEN_TOTAL, HEAD_TOTAL, PLAIN_QK_WIDTH + QK_ROPE)
    query_rope = rotate(query[..., PLAIN_QK_WIDTH:].astype(jnp.float32), rope_angles[:, None, :]).astype(jnp.bfloat16)
    key_expanded = key_up_weight.astype(jnp.float32).reshape(KEY_VALUE_RANK, HEAD_TOTAL, PLAIN_QK_WIDTH)
    query_latent = jnp.einsum('thd,lhd->thl', query[..., :PLAIN_QK_WIDTH].astype(jnp.float32), key_expanded).astype(jnp.bfloat16)
    latent_pre = jnp.dot(normed, latent_down_weight, preferred_element_type=jnp.float32)
    latent = (latent_pre * lax.rsqrt(lax.optimization_barrier(jnp.mean(latent_pre * latent_pre, axis=-1, keepdims=True)) + epsilon) * latent_norm_gain).astype(jnp.bfloat16)
    key_rope = rotate(jnp.dot(normed, w_rope_key, preferred_element_type=jnp.float32), rope_angles).astype(jnp.bfloat16)
    score_scale = (PLAIN_QK_WIDTH + QK_ROPE) ** (-0.5)
    query_block = min(512, TOKEN_TOTAL)
    key_index = jnp.arange(TOKEN_TOTAL, dtype=jnp.int32)
    latent_wide = latent.astype(jnp.float32)
    rope_wide = key_rope.astype(jnp.float32)

    def one_block(block_start):
        block_latent = lax.dynamic_slice_in_dim(query_latent, block_start, query_block, 0).astype(jnp.float32)
        block_rope = lax.dynamic_slice_in_dim(query_rope, block_start, query_block, 0).astype(jnp.float32)
        scores = (jnp.einsum('thl,kl->thk', block_latent, latent_wide) + jnp.einsum('thr,kr->thk', block_rope, rope_wide)) * score_scale
        query_index = block_start + jnp.arange(query_block, dtype=jnp.int32)
        allowed = key_index[None, None, :] <= query_index[:, None, None]
        scores = jnp.where(allowed, scores, masked_score)
        row_max = lax.optimization_barrier(jnp.max(scores, axis=-1))
        weights = jnp.where(allowed, jnp.exp(scores - row_max[..., None]), 0.0)
        weight_sum = lax.optimization_barrier(jnp.sum(weights, axis=-1))
        weighted = jnp.einsum('thk,kl->thl', weights.astype(jnp.bfloat16).astype(jnp.float32), latent_wide)
        return ((weighted / weight_sum[..., None]).astype(jnp.bfloat16), row_max + jnp.log(weight_sum))
    block_starts = jnp.arange(TOKEN_TOTAL // query_block, dtype=jnp.int32) * query_block
    latent_result, log_sums = lax.map(one_block, block_starts)
    latent_result = latent_result.reshape(TOKEN_TOTAL, HEAD_TOTAL, KEY_VALUE_RANK)
    log_sums = log_sums.reshape(TOKEN_TOTAL, HEAD_TOTAL)
    value_expanded = value_up_weight.astype(jnp.float32).reshape(KEY_VALUE_RANK, HEAD_TOTAL, VALUE_HEAD_WIDTH)
    attention = jnp.einsum('thl,lhv->thv', latent_result.astype(jnp.float32), value_expanded).astype(jnp.bfloat16).reshape(TOKEN_TOTAL, HEAD_TOTAL * VALUE_HEAD_WIDTH)
    channel_share = CC // N_TP
    head_share = HEAD_TOTAL * VALUE_HEAD_WIDTH // N_TP
    merged = jnp.zeros((TOKEN_TOTAL, MODEL_WIDTH), jnp.float32)
    for group_index in range(N_TP):
        channel_part = conv_out[:, group_index * channel_share:(group_index + 1) * channel_share]
        head_part = attention[:, group_index * head_share:(group_index + 1) * head_share]
        partial_value = jnp.dot(channel_part, w_merge_conv[group_index * channel_share:(group_index + 1) * channel_share], preferred_element_type=jnp.float32)
        partial_value = partial_value + jnp.dot(head_part, w_merge_attn[group_index * head_share:(group_index + 1) * head_share], preferred_element_type=jnp.float32)
        merged = merged + partial_value.astype(jnp.bfloat16).astype(jnp.float32)
    return (merged.astype(jnp.bfloat16), log_sums)
```

```python
import jax
import jax.numpy as jnp
from jax import lax
from jax.experimental import pallas as pl
from jax.experimental.pallas import tpu as pltpu
from jax.sharding import PartitionSpec as P

PLAIN_QK_WIDTH = 128
QK_ROPE = 64
VALUE_HEAD_WIDTH = 128

epsilon = 1e-06
rope_base = 10000.0
masked_score = -1e30
MESH = pl.DeviceIdType.MESH
ANY = pl.BlockSpec(memory_space=pl.ANY)


def angles_at(positions, width):
    inverse = rope_base ** (-2.0 * jnp.arange(width // 2, dtype=jnp.float32) / width)
    return positions[:, None] * inverse[None, :]


def rotate(halves, angle):
    middle = halves.shape[-1] // 2
    first, second = (halves[..., :middle], halves[..., middle:])
    cosine, sine = (jnp.cos(angle), jnp.sin(angle))
    return jnp.concatenate(
        [first * cosine - second * sine, first * sine + second * cosine], axis=-1
    )


class Place:
    def __init__(self, sp, tp, B):
        self.sp, self.tp, self.B, self.A = sp, tp, B, sp // B
        self.s = lax.axis_index("sp")
        self.t = lax.axis_index("tp")
        self.a = self.s // B
        self.b = lax.rem(self.s, B)

    def in_line(self, k):
        return {"sp": lax.rem(self.a + k, self.A) * self.B + self.b, "tp": self.t}

    def in_plane(self, k):
        return {"sp": self.a * self.B + lax.rem(self.b + k, self.B), "tp": self.t}

    def in_sp(self, k):
        return {"sp": lax.rem(self.s + k, self.sp), "tp": self.t}

    def in_tp(self, k):
        return {"sp": self.s, "tp": lax.rem(self.t + k, self.tp)}


def loop(start, stop, body):
    if stop > start:
        lax.fori_loop(start, stop, lambda k, c: (body(k), c)[1], 0)


def greet(groups):
    barrier = pltpu.get_barrier_semaphore()
    total = 0
    for where, count in groups:
        loop(
            1,
            count,
            lambda k: pl.semaphore_signal(
                barrier, inc=1, device_id=where(k), device_id_type=MESH
            ),
        )
        total += count - 1
    pl.semaphore_wait(barrier, total)


def remote(src, dst, send, recv, where):
    return pltpu.make_async_remote_copy(
        src_ref=src, dst_ref=dst, send_sem=send, recv_sem=recv, device_id=where,
        device_id_type=MESH,
    )


def stages(p, out, send, recv):
    line = lambda k: remote(
        out.at[p.a, p.b, p.t], out.at[p.a, p.b, p.t],
        send.at[0, k], recv.at[0, k], p.in_line(k))
    plane = lambda k: remote(
        out.at[:, p.b, p.t], out.at[:, p.b, p.t],
        send.at[1, k], recv.at[1, k], p.in_plane(k))
    pair = lambda k: remote(
        out.at[:, :, p.t], out.at[:, :, p.t],
        send.at[2, k], recv.at[2, k], p.in_tp(k))
    return line, plane, pair


def first_kernel(sp, tp, B, tok, wv, wg, wd, x, vo, go, do, local, tsend, trecv,
                 dsend, drecv, wsend, wrecv):
    p = Place(sp, tp, B)
    F = tok.shape[1]
    width = vo.shape[2]
    mine = pl.ds(pl.multiple_of(p.t * F, F), F)
    columns = lambda k: pl.ds(
        pl.multiple_of(lax.rem(lax.rem(p.s + k, sp), B) * width, width), width)
    greet([(p.in_sp, sp), (p.in_tp, tp)])
    own = [
        pltpu.make_async_copy(wd, do.at[p.a, p.b, p.t], local.at[0]),
        pltpu.make_async_copy(tok, x.at[p.b, :, mine], local.at[1]),
        pltpu.make_async_copy(wv.at[:, columns(0)], vo.at[p.s], local.at[2]),
        pltpu.make_async_copy(wg.at[:, columns(0)], go.at[p.s], local.at[3]),
    ]
    for copy in own:
        copy.start()
    tok_plane = lambda k: remote(
        tok, x.at[p.b, :, mine], tsend.at[0, k], trecv.at[0, k], p.in_plane(k))
    tok_pair = lambda k: remote(
        x.at[:, :, mine], x.at[:, :, mine], tsend.at[1, k], trecv.at[1, k], p.in_tp(k))
    value = lambda k: remote(
        wv.at[:, columns(k)], vo.at[p.s], wsend.at[0, k], wrecv.at[0, k], p.in_sp(k))
    gate = lambda k: remote(
        wg.at[:, columns(k)], go.at[p.s], wsend.at[1, k], wrecv.at[1, k], p.in_sp(k))
    line, plane, pair = stages(p, do, dsend, drecv)
    own[0].wait()
    loop(1, p.A, lambda k: line(k).start())
    loop(1, B, lambda k: tok_plane(k).start())
    loop(1, sp, lambda k: value(k).start())
    loop(1, p.A, lambda k: line(k).wait())
    loop(1, B, lambda k: plane(k).start())
    loop(1, sp, lambda k: gate(k).start())
    own[1].wait()
    loop(1, B, lambda k: tok_plane(k).wait())
    loop(1, tp, lambda k: tok_pair(k).start())
    loop(1, B, lambda k: plane(k).wait())
    loop(1, tp, lambda k: pair(k).start())
    loop(1, sp, lambda k: value(k).wait())
    loop(1, sp, lambda k: gate(k).wait())
    loop(1, tp, lambda k: tok_pair(k).wait())
    loop(1, tp, lambda k: pair(k).wait())
    own[2].wait()
    own[3].wait()


def gather_first(sp, tp, B, tok, wv, wg, wd):
    R, F = tok.shape
    D, C = wv.shape
    sds = jax.ShapeDtypeStruct
    D2 = pltpu.SemaphoreType.DMA
    most = max(sp // B, B, tp)
    return pl.pallas_call(
        lambda *refs: first_kernel(sp, tp, B, *refs),
        out_shape=(
            sds((B, R, tp * F), tok.dtype),
            sds((sp, D, C // B), wv.dtype),
            sds((sp, D, C // B), wg.dtype),
            sds((sp // B, B, tp) + wd.shape, wd.dtype),
        ),
        in_specs=[ANY] * 4,
        out_specs=(ANY,) * 4,
        scratch_shapes=[
            D2((4,)), D2((2, max(B, tp))), D2((2, max(B, tp))),
            D2((3, most)), D2((3, most)), D2((2, sp)), D2((2, sp)),
        ],
        compiler_params=pltpu.CompilerParams(collective_id=0, has_side_effects=True),
        name="gather_first",
    )(tok, wv, wg, wd)


def latent_kernel(sp, tp, B, block, out, local, send, recv):
    p = Place(sp, tp, B)
    greet([(p.in_line, p.A), (p.in_plane, B), (p.in_tp, tp)])
    own = pltpu.make_async_copy(block, out.at[p.a, p.b, p.t], local)
    own.start()
    own.wait()
    for part, count in zip(stages(p, out, send, recv), (p.A, B, tp)):
        loop(1, count, lambda k: part(k).start())
        loop(1, count, lambda k: part(k).wait())


def gather_latent(sp, tp, B, block):
    most = max(sp // B, B, tp)
    D2 = pltpu.SemaphoreType.DMA
    return pl.pallas_call(
        lambda *refs: latent_kernel(sp, tp, B, *refs),
        out_shape=jax.ShapeDtypeStruct((sp // B, B, tp) + block.shape, block.dtype),
        in_specs=[ANY],
        out_specs=ANY,
        scratch_shapes=[D2(()), D2((3, most)), D2((3, most))],
        compiler_params=pltpu.CompilerParams(collective_id=1, has_side_effects=True),
        name="gather_latent",
    )(block)


def swap_kernel(sp, tp, B, plane, blocks, out, local, send, recv):
    p = Place(sp, tp, B)
    n = B if plane else tp
    me = p.b if plane else p.t
    where = p.in_plane if plane else p.in_tp
    greet([(where, n)])
    own = pltpu.make_async_copy(blocks.at[me], out.at[me], local)
    own.start()
    copy = lambda k: remote(
        blocks.at[lax.rem(me + k, n)], out.at[me], send.at[k], recv.at[k], where(k))
    loop(1, n, lambda k: copy(k).start())
    loop(1, n, lambda k: copy(k).wait())
    own.wait()


def swap(sp, tp, B, plane, blocks, collective_id):
    D2 = pltpu.SemaphoreType.DMA
    n = B if plane else tp
    return pl.pallas_call(
        lambda *refs: swap_kernel(sp, tp, B, plane, *refs),
        out_shape=jax.ShapeDtypeStruct(blocks.shape, blocks.dtype),
        in_specs=[ANY],
        out_specs=ANY,
        scratch_shapes=[D2(()), D2((n,)), D2((n,))],
        compiler_params=pltpu.CompilerParams(
            collective_id=collective_id, has_side_effects=True),
        name="swap_plane" if plane else "swap_tp",
    )(blocks)


def norm_rows(features, gain):
    return (
        features
        * lax.rsqrt(jnp.mean(features * features, axis=-1, keepdims=True) + epsilon)
        * gain
    ).astype(jnp.bfloat16)


def local(
    tokens,
    norm_gain,
    w_value,
    w_gate,
    conv_taps,
    conv_gain,
    w_query,
    latent_down_weight,
    latent_norm_gain,
    w_rope_key,
    key_up_weight,
    value_up_weight,
    w_merge_conv,
    w_merge_attn,
):
    row_count = tokens.shape[0]
    sp = lax.axis_size("sp")
    tp = lax.axis_size("tp")
    C = w_value.shape[1]
    B = 1
    while B < 4 and sp % (2 * B) == 0 and C % (2 * B * 128) == 0:
        B *= 2
    s, t = lax.axis_index("sp"), lax.axis_index("tp")
    spot = lax.rem(s, B)
    latent_width = latent_down_weight.shape[1]

    down = jnp.concatenate([latent_down_weight, w_rope_key], axis=1)
    down_rows = down.shape[0] // tp
    down = lax.dynamic_slice_in_dim(down, t * down_rows, down_rows, 0)
    x, value_w, gate_w, down_w = gather_first(sp, tp, B, tokens, w_value, w_gate, down)
    features = x.shape[-1]
    x = x.reshape(B * row_count, features)
    normed = norm_rows(x.astype(jnp.float32), norm_gain)
    own = lax.dynamic_slice_in_dim(normed, spot * row_count, row_count, 0)
    first_row = s * row_count
    query_index = first_row + jnp.arange(row_count, dtype=jnp.int32)
    slice_rows = row_count // tp
    slice_start = t * slice_rows
    key_rows = lax.dynamic_slice_in_dim(own, slice_start, slice_rows, 0)
    key_index = first_row + slice_start + jnp.arange(slice_rows, dtype=jnp.int32)
    down_pre = jnp.dot(
        key_rows, down_w.reshape(features, -1), preferred_element_type=jnp.float32
    )
    latent = norm_rows(down_pre[:, :latent_width], latent_norm_gain)
    key_rope = rotate(
        down_pre[:, latent_width:], angles_at(key_index.astype(jnp.float32), QK_ROPE)
    ).astype(jnp.bfloat16)
    keys = gather_latent(sp, tp, B, jnp.concatenate([latent, key_rope], axis=1))
    keys = keys.reshape(sp * row_count, -1)

    value_pre = jnp.dot(
        normed, value_w.reshape(features, -1), preferred_element_type=jnp.float32
    )
    gate_pre = jnp.dot(
        normed, gate_w.reshape(features, -1), preferred_element_type=jnp.float32
    )
    gated = (value_pre * jax.nn.sigmoid(gate_pre)).astype(jnp.bfloat16)
    rows, width = gated.shape
    reach = conv_taps.shape[0] - 1
    prior, back = [], 1
    while sum(q.shape[0] for q in prior) < reach:
        need = min(rows, reach - sum(q.shape[0] for q in prior))
        route = [(i - back * B, i) for i in range(back * B, sp)]
        prior.insert(0, lax.ppermute(gated[rows - need :], "sp", route))
        back += 1
    padded = jnp.concatenate(prior + [gated], axis=0).astype(jnp.float32)
    taps = lax.dynamic_slice_in_dim(conv_taps, spot * width, width, 1).astype(jnp.float32)
    mixed = jnp.zeros(gated.shape, jnp.float32)
    for tap_index in range(reach + 1):
        mixed = mixed + taps[tap_index] * padded[tap_index : tap_index + rows]
    mixed = swap(sp, tp, B, True, mixed.astype(jnp.bfloat16).reshape(B, row_count, width), 2)
    mixed = mixed.astype(jnp.float32)
    stat_sum, stat_squares = lax.psum(
        (jnp.sum(mixed, axis=(0, 2)), jnp.sum(mixed * mixed, axis=(0, 2))), "tp"
    )
    channel_total = C * tp
    channel_mean = stat_sum / channel_total
    channel_var = stat_squares / channel_total - channel_mean * channel_mean
    conv_out = jax.nn.silu(
        (mixed - channel_mean[None, :, None])
        * lax.rsqrt(channel_var + epsilon)[None, :, None]
        * conv_gain.reshape(B, 1, width)
    ).astype(jnp.bfloat16)

    head_count = key_up_weight.shape[1] // PLAIN_QK_WIDTH
    query = (
        jnp.dot(own, w_query, preferred_element_type=jnp.float32)
        .astype(jnp.bfloat16)
        .reshape(row_count, head_count, PLAIN_QK_WIDTH + QK_ROPE)
    )
    query_angles = angles_at(query_index.astype(jnp.float32), QK_ROPE)
    query_rope = rotate(
        query[..., PLAIN_QK_WIDTH:].astype(jnp.float32), query_angles[:, None, :]
    ).astype(jnp.bfloat16)
    key_expanded = key_up_weight.reshape(latent_width, head_count, PLAIN_QK_WIDTH)
    query_latent = jnp.einsum(
        "thd,lhd->thl",
        query[..., :PLAIN_QK_WIDTH],
        key_expanded,
        preferred_element_type=jnp.float32,
    ).astype(jnp.bfloat16)
    score_scale = (PLAIN_QK_WIDTH + QK_ROPE) ** (-0.5)
    scores = (
        jnp.einsum(
            "thl,kl->thk",
            jnp.concatenate([query_latent, query_rope], axis=-1),
            keys,
            preferred_element_type=jnp.float32,
        )
        * score_scale
    )
    key_at = jnp.arange(keys.shape[0], dtype=jnp.int32)
    allowed = key_at[None, None, :] <= query_index[:, None, None]
    scores = jnp.where(allowed, scores, masked_score)
    row_max = jnp.max(scores, axis=-1)
    weights = jnp.where(allowed, jnp.exp(scores - row_max[..., None]), 0.0)
    weight_sum = jnp.sum(weights, axis=-1)
    weighted = jnp.einsum(
        "thk,kl->thl",
        weights.astype(jnp.bfloat16),
        keys[:, :latent_width],
        preferred_element_type=jnp.float32,
    )
    latent_result = (weighted / weight_sum[..., None]).astype(jnp.bfloat16)
    log_sums = row_max + jnp.log(weight_sum)
    value_expanded = value_up_weight.reshape(latent_width, head_count, VALUE_HEAD_WIDTH)
    attention = (
        jnp.einsum(
            "thl,lhv->thv", latent_result, value_expanded, preferred_element_type=jnp.float32
        )
        .astype(jnp.bfloat16)
        .reshape(row_count, head_count * VALUE_HEAD_WIDTH)
    )
    partial = (
        jnp.einsum(
            "btc,bcm->tm",
            conv_out,
            w_merge_conv.reshape(B, width, -1),
            preferred_element_type=jnp.float32,
        )
        + jnp.dot(attention, w_merge_attn, preferred_element_type=jnp.float32)
    ).astype(jnp.bfloat16)
    parts = swap(sp, tp, B, False, partial.reshape(tp, slice_rows, -1), 3)
    merged = jnp.sum(parts.astype(jnp.float32), axis=0).astype(jnp.bfloat16)
    return (merged, log_sums)


def solution(mesh):
    return jax.shard_map(
        local,
        mesh=mesh,
        in_specs=(
            P("sp", "tp"),
            P(),
            P("sp", "tp"),
            P("sp", "tp"),
            P(None, "tp"),
            P("tp"),
            P(None, "tp"),
            P("sp", None),
            P(),
            P("sp", None),
            P(None, "tp"),
            P(None, "tp"),
            P("tp", None),
            P("tp", None),
        ),
        out_specs=(P(("sp", "tp"), None), P("sp", "tp")),
        check_vma=False,
    )
```
